32 devices in a mesh: ep: 8 (over z, y), tp: 4 (over x, core).
Axes of the slice: x: 2, y: 2, z: 4, core: 2. Of those that a mesh axis runs over, the one named last changes fastest.
Arguments:
- tokens: bfloat16 [2048, 2048], P('ep'), may hold values from -6 to 6
- expert_ids: int32 [2048, 2], P('ep'), may hold values from 0 to 7, all different within a row; in each aligned block of 256 rows (0 to 255, 256 to 511, ...) at most 192 rows name the same one
- route_weight: float32 [2048, 2], P('ep'), may hold values from 0.1 to 1
- norm_gain: float32 [2048], replicated, may hold values from 0.1 to 1.9
- expert_gate: bfloat16 [8, 2048, 2048], P('ep', None, 'tp'), may hold values from -4 to 4
- expert_up: bfloat16 [8, 2048, 2048], P('ep', None, 'tp'), may hold values from -4 to 4
- expert_down: bfloat16 [8, 2048, 2048], P('ep', 'tp'), may hold values from -0.03125 to 0.03125
Outputs:
- combined: bfloat16 [2048, 2048], P('ep', 'tp')
The draws below stay inside these ranges and needn't reach their ends.
Inputs may be any that keep to these rules, and one draw needn't show every extreme that they name: `expert_ids`: each row names 2 different experts. In each aligned block of 256 rows (the rows of one index of ep) no expert is named by more than 192 rows, and in some block one expert is named by exactly 192 rows.
All inputs are finite; a program needn't handle non-finite values.
Results may differ from the reference program's by a relative error of at most 0.012.
Values may be sent and summed in bfloat16 or wider, within the bound.
A program may use at most 128 MiB of HBM per device.

```python
import math
import jax
import jax.numpy as jnp
import numpy as np
from jax import lax

D = 2048
FF = 2048
TOP_K = 2
TOK_GROUP = 256
EXPERTS = 8
TOKENS = 2048
CAP = 192
N_EP = 8
N_TP = 4


def draw_expert_gate(key, part):
    spread = 3.0
    normal_draw = jax.random.truncated_normal(jax.random.fold_in(key, 11), -4.0, 4.0, (EXPERTS, D, FF), jnp.float32)
    return (normal_draw * (spread / math.sqrt(D))).astype(jnp.bfloat16)


def draw_expert_up(key, part):
    spread = 3.0
    normal_draw = jax.random.truncated_normal(jax.random.fold_in(key, 23), -4.0, 4.0, (EXPERTS, D, FF), jnp.float32)
    return (normal_draw * (spread / math.sqrt(D))).astype(jnp.bfloat16)


def shard_levels(rng, shape, shards, least, largest):
    gain = 1.0
    for dim, blocks in shards:
        draws = jax.random.uniform(jax.random.fold_in(jax.random.fold_in(rng, 6), dim), (blocks,), jnp.float32, least / len(shards), largest / len(shards))
        gain = gain * jnp.repeat(jnp.exp(draws), shape[dim] // blocks).reshape((-1,) + (1,) * (len(shape) - 1 - dim))
    return gain


def routed_block(own_key, own, number, rows, amount, top, limit, skew):
    order = jax.random.permutation(own_key, amount)
    heavy_load, ordinary = portions_of(amount, rows * top, limit, skew, True), portions_of(amount, rows * top, limit, skew, False)
    places = jnp.arange(amount)

    def named(tallies, rotation):
        used = int((tallies > 0).sum())
        fixed = max(1, used // 4)
        shifted = fixed + (places - fixed + rotation * (used - fixed)) % max(1, amount - fixed)
        return jnp.zeros((amount,), jnp.int32).at[order[jnp.where(places < fixed, places, shifted)]].set(jnp.asarray(tallies, jnp.int32))

    tallies = jnp.where(number % 4 == 0, named(heavy_load, number // 4), named(ordinary, number - number // 4 - 1))
    mixed = jax.random.permutation(jax.random.fold_in(own, 3), amount)
    giver, sink = mixed[0:amount // 2 * 2:2], mixed[1:amount // 2 * 2:2]
    room = jnp.minimum(tallies[giver] - 1, limit - tallies[sink]) // 2
    room = jnp.where((giver == order[0]) | (sink == order[0]) | (tallies[sink] == 0), 0, jnp.maximum(room, 0))
    shifted = jax.random.randint(jax.random.fold_in(own, 4), (amount // 2,), 0, 1 << 20) % (room + 1)
    tallies = tallies.at[giver].add(-shifted).at[sink].add(shifted)
    labels = jnp.searchsorted(jnp.cumsum(tallies), jnp.arange(rows * top), side="right").astype(jnp.int32)
    table = labels.reshape(top, rows).T
    table = table[jax.random.permutation(jax.random.fold_in(own, 1), rows)]
    rotation = jax.random.randint(jax.random.fold_in(own, 2), (rows, 1), 0, top)
    return jnp.take_along_axis(table, (jnp.arange(top)[None, :] + rotation) % top, axis=1)


def portions_of(count, total, most, skew, full):
    loads = [(1 << 20) // math.isqrt(grade ** skew) + 1 for grade in range(1, count + 1)]
    largest = most if full else min(most, max(-(-total // count), total * loads[0] // sum(loads)))
    least = 1 if total - largest >= count - 1 else 0
    counts, surplus = [largest] + [least] * (count - 1), total - largest - least * (count - 1)
    while surplus > 0:
        candidates = [i for i in range(1, count) if counts[i] < largest] or [i for i in range(1, count) if counts[i] < most]
        mass, remaining = sum([loads[i] for i in candidates]), surplus
        for i in candidates:
            more = min(most - counts[i], max(1, remaining * loads[i] // mass), surplus)
            counts[i] = counts[i] + more
            surplus = surplus - more
    return np.array(counts)


def bell_draw(key, shape, scale, most, pieces=(), kind=jnp.bfloat16):
    result = jax.random.normal(key, shape, jnp.float32) * scale
    if len(pieces) > 0:
        result = shard_levels(key, shape, pieces, -0.22, 0.18) * result
    return jnp.clip(result, min=-most, max=most).astype(kind)


def setup_inputs(seed: int = 0) -> dict:
    key_list = jax.random.split(jax.random.key(seed), 8)
    tokens = bell_draw(key_list[0], (TOKENS, D), 1.0, 6.0, ((0, 8),))
    expert_ids_keys = jax.random.split(jax.random.fold_in(key_list[1], 1), TOKENS // TOK_GROUP)
    expert_ids_turns = jax.random.permutation(jax.random.fold_in(key_list[1], 3), TOKENS // TOK_GROUP)
    expert_ids = jax.vmap(lambda own, number: routed_block(jax.random.fold_in(key_list[1], 2), own, number, TOK_GROUP, EXPERTS, TOP_K, CAP, 1))(expert_ids_keys, expert_ids_turns).reshape((TOKENS, TOP_K))
    route_weight = jnp.clip(0.1 + 0.9 * jax.random.uniform(key_list[2], (TOKENS, TOP_K), jnp.float32) ** shard_levels(key_list[2], (TOKENS, TOP_K), ((0, 8),), -0.2, 0.2), 0.1, 1.0)
    norm_gain = jnp.clip(1.0 + 0.18 * jax.random.normal(key_list[3], (D,), jnp.float32), 0.1, 1.9)
    expert_gate = draw_expert_gate(jax.random.fold_in(key_list[7], 71), 0)
    expert_up = draw_expert_up(jax.random.fold_in(key_list[7], 71), 0)
    expert_down = bell_draw(key_list[6], (EXPERTS, FF, D), (16 * FF) ** -0.5, 0.03125, ((0, 8), (1, 4)))
    return dict(tokens=tokens, expert_ids=expert_ids, route_weight=route_weight, norm_gain=norm_gain, expert_gate=expert_gate, expert_up=expert_up, expert_down=expert_down)


NORM_EPS = 1e-06
CLAMP_LIMIT = 7.0
SWISH_SCALE = 1.702

def normalize(tokens, norm_gain):
    values = tokens.astype(jnp.float32)
    scaled = values * lax.rsqrt(lax.optimization_barrier(jnp.mean(values * values, axis=-1, keepdims=True)) + NORM_EPS)
    return (scaled * norm_gain).astype(jnp.bfloat16)

def activate(gate_sum, up_sum):
    gate_cut = jnp.minimum(gate_sum, CLAMP_LIMIT)
    up_cut = jnp.clip(up_sum, -CLAMP_LIMIT, CLAMP_LIMIT)
    return ((up_cut + 1.0) * gate_cut * jax.nn.sigmoid(SWISH_SCALE * gate_cut)).astype(jnp.bfloat16)

def reference(tokens, expert_ids, route_weight, norm_gain, expert_gate, expert_up, expert_down):
    normed = normalize(tokens, norm_gain)
    flat_ids = expert_ids.reshape(N_EP, TOK_GROUP * TOP_K)
    onehot = (flat_ids[:, :, None] == jnp.arange(EXPERTS, dtype=jnp.int32)[None, None, :]).astype(jnp.int32)
    slot_index = lax.optimization_barrier(jnp.sum(jnp.cumsum(onehot, axis=1) * onehot, axis=2)) - 1
    block_index = jnp.arange(N_EP, dtype=jnp.int32)[:, None]
    token_index = block_index * TOK_GROUP + jnp.arange(TOK_GROUP * TOP_K, dtype=jnp.int32)[None, :] // TOP_K
    position = (block_index * CAP + slot_index).astype(jnp.int32)
    row_table = jnp.full((EXPERTS, N_EP * CAP), TOKENS, jnp.int32).at[flat_ids, position].set(token_index.astype(jnp.int32))
    padded = jnp.concatenate([normed, jnp.zeros((1, D), jnp.bfloat16)], axis=0)
    quarter = FF // N_TP

    def one_expert(operands):
        rows_index, gate_w, up_w, down_w = operands
        picked = padded[rows_index]
        gate_sum = jnp.dot(picked, gate_w, preferred_element_type=jnp.float32)
        up_sum = jnp.dot(picked, up_w, preferred_element_type=jnp.float32)
        activated = activate(gate_sum, up_sum)
        total_sum = jnp.zeros((picked.shape[0], D), jnp.float32)
        for shard_number in range(N_TP):
            lower = shard_number * quarter
            partial_value = jnp.dot(activated[:, lower:lower + quarter], down_w[lower:lower + quarter], preferred_element_type=jnp.float32)
            rounded = lax.optimization_barrier(partial_value.astype(jnp.bfloat16))
            total_sum = total_sum + rounded.astype(jnp.float32)
        return total_sum.astype(jnp.bfloat16)
    outputs = lax.map(one_expert, (row_table, expert_gate, expert_up, expert_down))
    flat_out = outputs.reshape(EXPERTS * N_EP * CAP, D)
    out_index = (flat_ids * (N_EP * CAP) + position).reshape(-1)
    chosen = flat_out[out_index].reshape(TOKENS, TOP_K, D).astype(jnp.float32)
    combined = lax.optimization_barrier(jnp.sum(chosen * route_weight[:, :, None], axis=1))
    return combined.astype(jnp.bfloat16)
```

```python
import functools

import jax
import jax.numpy as jnp
from jax import lax
from jax.experimental import pallas as pl
from jax.experimental.pallas import tpu as pltpu
from jax.sharding import PartitionSpec as P

NORM_EPS = 1e-06
CLAMP_LIMIT = 7.0
SWISH_SCALE = 1.702
MESH = pl.DeviceIdType.MESH


def activate(gate_sum, up_sum):
    gate_cut = jnp.minimum(gate_sum, CLAMP_LIMIT)
    up_cut = jnp.clip(up_sum, -CLAMP_LIMIT, CLAMP_LIMIT)
    return ((up_cut + 1.0) * gate_cut * jax.nn.sigmoid(SWISH_SCALE * gate_cut)).astype(jnp.bfloat16)


def expert_kernel(
    groups,
    send,
    gate_hbm,
    up_hbm,
    down_hbm,
    out,
    gate_w,
    up_w,
    down_w,
    rows,
    part,
    pair_in,
    cross_out,
    cross_in,
    result,
    w_sem,
    disp_send,
    disp_recv,
    cross_send,
    cross_recv,
    core_send,
    core_recv,
    fwd_send,
    fwd_recv,
    pair_send,
    pair_recv,
    sum_send,
    sum_recv,
    ret_send,
    ret_recv,
):
    me = lax.axis_index("ep")
    tp = lax.axis_index("tp")
    a, b = tp // 2, lax.rem(tp, 2)
    cross = 2 * (1 - a) + b
    core = 2 * a + 1 - b
    quarter = send.shape[2]

    weights = [
        pltpu.make_async_copy(src, dst, w_sem.at[i])
        for i, (src, dst) in enumerate(((gate_hbm, gate_w), (up_hbm, up_w), (down_hbm, down_w)))
    ]

    def remote(src, dst, send_sem, recv_sem, ep_index, tp_index):
        return pltpu.make_async_remote_copy(
            src_ref=src,
            dst_ref=dst,
            send_sem=send_sem,
            recv_sem=recv_sem,
            device_id=(ep_index, tp_index),
            device_id_type=MESH,
        )

    def dispatch(k):
        dst = lax.rem(me + k, groups)
        return remote(send.at[dst], rows.at[k, tp], disp_send.at[k], disp_recv.at[k], dst, tp)

    def dispatch_own():
        return pltpu.make_async_copy(send.at[me], rows.at[0, tp], disp_recv.at[0])

    def to_cross(k):
        return remote(rows.at[k, tp], rows.at[k, tp], cross_send.at[k], cross_recv.at[k], me, cross)

    def to_core(k):
        return remote(rows.at[k, tp], rows.at[k, tp], core_send.at[k], core_recv.at[k], me, core)

    def forward(k):
        return remote(rows.at[k, cross], rows.at[k, cross], fwd_send.at[k], fwd_recv.at[k], me, core)

    def pair(k):
        return remote(part.at[k, 1 - b], pair_in.at[k], pair_send.at[k], pair_recv.at[k], me, core)

    def cross_sum(k):
        return remote(cross_out.at[k], cross_in.at[k], sum_send.at[k], sum_recv.at[k], me, cross)

    def give_back(k):
        src = lax.rem(me + groups - k, groups)
        return remote(result.at[k], out.at[me], ret_send.at[k], ret_recv.at[k], src, tp)

    def give_back_own():
        return pltpu.make_async_copy(result.at[0], out.at[me], ret_recv.at[0])

    for copy in weights:
        copy.start()
    dispatch_own().start()

    barrier = pltpu.get_barrier_semaphore()

    def greet(k, carry):
        pl.semaphore_signal(
            barrier, inc=1, device_id=(lax.rem(me + k, groups), tp), device_id_type=MESH
        )
        return carry

    lax.fori_loop(1, groups, greet, 0)
    pl.semaphore_signal(barrier, inc=1, device_id=(me, cross), device_id_type=MESH)
    pl.semaphore_signal(barrier, inc=1, device_id=(me, core), device_id_type=MESH)
    pl.semaphore_wait(barrier, groups + 1)

    def launch(k, carry):
        dispatch(k).start()
        return carry

    lax.fori_loop(1, groups, launch, 0)
    for copy in weights:
        copy.wait()

    def step(i, carry):
        @pl.when(i < groups)
        def _():
            @pl.when(i == 0)
            def _():
                dispatch_own().wait()

            @pl.when(i > 0)
            def _():
                dispatch(i).wait_recv()

            to_cross(i).start()
            to_core(i).start()

        @pl.when((i >= 1) & (i < groups + 1))
        def _():
            k = i - 1
            to_cross(k).wait_recv()
            forward(k).start()

        @pl.when((i >= 3) & (i < groups + 3))
        def _():
            k = i - 3
            pair(k).wait_recv()
            total = part[k, b, 1 - a].astype(jnp.float32) + pair_in[k, 1 - a].astype(jnp.float32)
            cross_out[k] = total.astype(jnp.bfloat16)
            cross_sum(k).start()

        @pl.when((i >= 2) & (i < groups + 2))
        def _():
            k = i - 2
            to_core(k).wait_recv()
            forward(k).wait_recv()
            block = jnp.concatenate([rows[k, j] for j in range(4)], axis=1)
            gate_sum = jnp.dot(block, gate_w[...], preferred_element_type=jnp.float32)
            up_sum = jnp.dot(block, up_w[...], preferred_element_type=jnp.float32)
            activated = activate(gate_sum, up_sum)
            for j in range(4):
                part[k, j % 2, j // 2] = jnp.dot(
                    activated,
                    down_w[:, j * quarter : (j + 1) * quarter],
                    preferred_element_type=jnp.float32,
                ).astype(jnp.bfloat16)
            pair(k).start()

        @pl.when(i >= 4)
        def _():
            k = i - 4
            cross_sum(k).wait_recv()
            total = part[k, b, a].astype(jnp.float32) + pair_in[k, a].astype(jnp.float32)
            result[k] = (total + cross_in[k].astype(jnp.float32)).astype(jnp.bfloat16)

            @pl.when(k == 0)
            def _():
                give_back_own().start()

            @pl.when(k > 0)
            def _():
                give_back(k).start()

        return carry

    lax.fori_loop(0, groups + 4, step, 0)

    def finish(k, carry):
        to_cross(k).wait_send()
        to_core(k).wait_send()
        forward(k).wait_send()
        pair(k).wait_send()
        cross_sum(k).wait_send()

        @pl.when(k == 0)
        def _():
            give_back_own().wait()

        @pl.when(k > 0)
        def _():
            dispatch(k).wait_send()
            give_back(k).wait_send()
            give_back(k).wait_recv()

        return carry

    lax.fori_loop(0, groups, finish, 0)


def run_experts(send, gate_w, up_w, down_w):
    groups, capacity, quarter = send.shape
    bf16 = jnp.bfloat16
    sems = [pltpu.SemaphoreType.DMA((groups,)) for _ in range(14)]
    return pl.pallas_call(
        functools.partial(expert_kernel, groups),
        out_shape=jax.ShapeDtypeStruct(send.shape, bf16),
        in_specs=[pl.BlockSpec(memory_space=pltpu.VMEM)] + [pl.BlockSpec(memory_space=pl.ANY)] * 3,
        out_specs=pl.BlockSpec(memory_space=pltpu.VMEM),
        scratch_shapes=[
            pltpu.VMEM(gate_w.shape, bf16),
            pltpu.VMEM(up_w.shape, bf16),
            pltpu.VMEM(down_w.shape, bf16),
            pltpu.VMEM((groups, 4, capacity, quarter), bf16),
            pltpu.VMEM((groups, 2, 2, capacity, quarter), bf16),
            pltpu.VMEM((groups, 2, capacity, quarter), bf16),
            pltpu.VMEM(send.shape, bf16),
            pltpu.VMEM(send.shape, bf16),
            pltpu.VMEM(send.shape, bf16),
            pltpu.SemaphoreType.DMA((3,)),
            *sems,
        ],
        compiler_params=pltpu.CompilerParams(
            collective_id=0, has_side_effects=True, vmem_limit_bytes=56 * 1024 * 1024
        ),
    )(send, gate_w, up_w, down_w)


def shards(tokens, expert_ids, route_weight, norm_gain, expert_gate, expert_up, expert_down):
    groups = lax.axis_size("ep")
    tp_count = lax.axis_size("tp")
    experts = groups * expert_gate.shape[0]
    tok_count, model_width = tokens.shape
    top_count = expert_ids.shape[1]
    capacity = min(tok_count, 3 * tok_count * top_count // experts)
    quarter = model_width // tp_count
    offset = lax.axis_index("tp") * quarter

    values = tokens.astype(jnp.float32)
    scale = lax.rsqrt(jnp.mean(values * values, axis=-1, keepdims=True) + NORM_EPS)
    own = lax.dynamic_slice_in_dim(tokens, offset, quarter, 1).astype(jnp.float32)
    own_gain = lax.dynamic_slice_in_dim(norm_gain, offset, quarter, 0)
    normed = (own * scale * own_gain).astype(jnp.bfloat16)

    onehot = expert_ids[:, :, None] == jnp.arange(experts, dtype=jnp.int32)
    named = jnp.any(onehot, axis=1).astype(jnp.bfloat16)
    order = jnp.arange(tok_count, dtype=jnp.int32)
    earlier = (order[None, :] < order[:, None]).astype(jnp.bfloat16)
    slots = jnp.dot(earlier, named, preferred_element_type=jnp.float32).astype(jnp.int32)
    slot_index = jnp.sum(jnp.where(onehot, slots[:, None, :], 0), axis=2)
    position = expert_ids * capacity + slot_index
    match = position[:, :, None] == jnp.arange(experts * capacity, dtype=jnp.int32)
    chosen = jnp.any(match, axis=1).astype(jnp.bfloat16)
    send = lax.dot_general(
        chosen, normed, (((0,), (0,)), ((), ())), preferred_element_type=jnp.float32
    ).astype(jnp.bfloat16)

    returned = run_experts(
        send.reshape(groups, capacity, quarter), expert_gate[0], expert_up[0], expert_down[0]
    ).reshape(experts * capacity, quarter)

    mix = jnp.sum(jnp.where(match, route_weight[:, :, None], 0.0), axis=1)
    high = lax.reduce_precision(mix, 8, 7)
    low = (mix - high).astype(jnp.bfloat16)
    combined = jnp.dot(high.astype(jnp.bfloat16), returned, preferred_element_type=jnp.float32)
    combined += jnp.dot(low, returned, preferred_element_type=jnp.float32)
    return combined.astype(jnp.bfloat16)


def solution(mesh):
    return jax.shard_map(
        shards,
        mesh=mesh,
        in_specs=(
            P("ep", None),
            P("ep", None),
            P("ep", None),
            P(),
            P("ep", None, "tp"),
            P("ep", None, "tp"),
            P("ep", "tp", None),
        ),
        out_specs=P("ep", "tp"),
        check_vma=False,
    )
```

```python
import functools

import jax
import jax.numpy as jnp
from jax import lax
from jax.experimental import pallas as pl
from jax.experimental.pallas import tpu as pltpu
from jax.sharding import PartitionSpec as P

NORM_EPS = 1e-06
CLAMP_LIMIT = 7.0
SWISH_SCALE = 1.702
MESH = pl.DeviceIdType.MESH


def activate(gate_sum, up_sum):
    gate_cut = jnp.minimum(gate_sum, CLAMP_LIMIT)
    up_cut = jnp.clip(up_sum, -CLAMP_LIMIT, CLAMP_LIMIT)
    return ((up_cut + 1.0) * gate_cut * jax.nn.sigmoid(SWISH_SCALE * gate_cut)).astype(jnp.bfloat16)


def expert_kernel(
    groups,
    send,
    send_cross,
    gate_hbm,
    up_hbm,
    down_hbm,
    out,
    gate_w,
    up_w,
    down_w,
    rows,
    part,
    pair_in,
    cross_out,
    cross_in,
    result,
    w_sem,
    disp_send,
    disp_recv,
    cross_send,
    cross_recv,
    core_send,
    core_recv,
    fwd_send,
    fwd_recv,
    pair_send,
    pair_recv,
    sum_send,
    sum_recv,
    ret_send,
    ret_recv,
):
    me = lax.axis_index("ep")
    tp = lax.axis_index("tp")
    a, b = tp // 2, lax.rem(tp, 2)
    cross = 2 * (1 - a) + b
    core = 2 * a + 1 - b
    quarter = send.shape[2]
    half = groups // 2

    weights = [
        pltpu.make_async_copy(src, dst, w_sem.at[i])
        for i, (src, dst) in enumerate(((gate_hbm, gate_w), (up_hbm, up_w), (down_hbm, down_w)))
    ]

    def remote(src, dst, send_sem, recv_sem, ep_index, tp_index):
        return pltpu.make_async_remote_copy(
            src_ref=src,
            dst_ref=dst,
            send_sem=send_sem,
            recv_sem=recv_sem,
            device_id=(ep_index, tp_index),
            device_id_type=MESH,
        )

    def partner(k):
        total, bit = 0, 1
        while bit < groups:
            total += bit * lax.rem(me // bit + k // bit, 2)
            bit *= 2
        return total

    def order(i):
        i = i + (i // (groups - 2)) * (1 - 2 * lax.rem(i, 2))
        return i // 2 + half * lax.rem(i, 2)

    def dispatch(k):
        dst = partner(k)
        return remote(send.at[dst], rows.at[k, tp], disp_send.at[k], disp_recv.at[k], dst, tp)

    def dispatch_own():
        return pltpu.make_async_copy(send.at[me], rows.at[0, tp], disp_recv.at[0])

    def dispatch_cross(k):
        dst = partner(k)
        return remote(
            send_cross.at[lax.rem(dst, half)],
            rows.at[k, cross],
            cross_send.at[k],
            cross_recv.at[k],
            dst,
            tp,
        )

    def dispatch_own_cross():
        return pltpu.make_async_copy(
            send_cross.at[lax.rem(me, half)], rows.at[0, cross], cross_recv.at[0]
        )

    def to_cross(k):
        return remote(rows.at[k, tp], rows.at[k, tp], cross_send.at[k], cross_recv.at[k], me, cross)

    def to_core(k):
        return remote(rows.at[k, tp], rows.at[k, tp], core_send.at[k], core_recv.at[k], me, core)

    def forward(k):
        return remote(rows.at[k, cross], rows.at[k, cross], fwd_send.at[k], fwd_recv.at[k], me, core)

    def pair(k):
        return remote(part.at[k, 1 - b], pair_in.at[k], pair_send.at[k], pair_recv.at[k], me, core)

    def cross_sum(k):
        return remote(cross_out.at[k], cross_in.at[k], sum_send.at[k], sum_recv.at[k], me, cross)

    def give_back(k):
        return remote(result.at[k], out.at[me], ret_send.at[k], ret_recv.at[k], partner(k), tp)

    def give_back_own():
        return pltpu.make_async_copy(result.at[0], out.at[me], ret_recv.at[0])

    for copy in weights:
        copy.start()
    dispatch_own().start()
    dispatch_own_cross().start()

    barrier = pltpu.get_barrier_semaphore()

    def greet(k, carry):
        pl.semaphore_signal(
            barrier, inc=1, device_id=(lax.rem(me + k, groups), tp), device_id_type=MESH
        )
        return carry

    lax.fori_loop(1, groups, greet, 0)
    pl.semaphore_signal(barrier, inc=1, device_id=(me, cross), device_id_type=MESH)
    pl.semaphore_signal(barrier, inc=1, device_id=(me, core), device_id_type=MESH)
    pl.semaphore_wait(barrier, groups + 1)

    def launch(i, carry):
        k = order(i)
        dispatch(k).start()

        @pl.when(k < half)
        def _():
            dispatch_cross(k).start()

        return carry

    lax.fori_loop(1, groups, launch, 0)
    for copy in weights:
        copy.wait()

    def step(i, carry):
        @pl.when(i >= 4)
        def _():
            k = order(i - 4)
            cross_sum(k).wait_recv()
            total = part[k, b, a].astype(jnp.float32) + pair_in[k, a].astype(jnp.float32)
            result[k] = (total + cross_in[k].astype(jnp.float32)).astype(jnp.bfloat16)

            @pl.when(k == 0)
            def _():
                give_back_own().start()

            @pl.when(k > 0)
            def _():
                give_back(k).start()

        @pl.when((i >= 3) & (i < groups + 3))
        def _():
            k = order(i - 3)
            pair(k).wait_recv()
            total = part[k, b, 1 - a].astype(jnp.float32) + pair_in[k, 1 - a].astype(jnp.float32)
            cross_out[k] = total.astype(jnp.bfloat16)
            cross_sum(k).start()

        @pl.when((i >= 2) & (i < groups + 2))
        def _():
            k = order(i - 2)
            to_core(k).wait_recv()
            forward(k).wait_recv()
            block = jnp.concatenate([rows[k, j] for j in range(4)], axis=1)
            gate_sum = jnp.dot(block, gate_w[...], preferred_element_type=jnp.float32)
            up_sum = jnp.dot(block, up_w[...], preferred_element_type=jnp.float32)
            activated = activate(gate_sum, up_sum)
            for j in range(4):
                part[k, j % 2, j // 2] = jnp.dot(
                    activated,
                    down_w[:, j * quarter : (j + 1) * quarter],
                    preferred_element_type=jnp.float32,
                ).astype(jnp.bfloat16)
            pair(k).start()

        @pl.when((i >= 1) & (i < groups + 1))
        def _():
            k = order(i - 1)

            @pl.when(k == 0)
            def _():
                dispatch_own_cross().wait()

            @pl.when(k > 0)
            def _():
                to_cross(k).wait_recv()

            forward(k).start()

        @pl.when(i < groups)
        def _():
            k = order(i)

            @pl.when(k == 0)
            def _():
                dispatch_own().wait()

            @pl.when(k > 0)
            def _():
                dispatch(k).wait_recv()

            @pl.when(k >= half)
            def _():
                to_cross(k).start()

            to_core(k).start()

        return carry

    lax.fori_loop(0, groups + 4, step, 0)

    def finish(k, carry):
        to_core(k).wait_send()
        forward(k).wait_send()
        pair(k).wait_send()
        cross_sum(k).wait_send()

        @pl.when(k == 0)
        def _():
            give_back_own().wait()

        @pl.when(k > 0)
        def _():
            to_cross(k).wait_send()
            dispatch(k).wait_send()
            give_back(k).wait_send()
            give_back(k).wait_recv()

        return carry

    lax.fori_loop(0, groups, finish, 0)


def run_experts(send, send_cross, gate_w, up_w, down_w):
    groups, capacity, quarter = send.shape
    bf16 = jnp.bfloat16
    sems = [pltpu.SemaphoreType.DMA((groups,)) for _ in range(14)]
    return pl.pallas_call(
        functools.partial(expert_kernel, groups),
        out_shape=jax.ShapeDtypeStruct(send.shape, bf16),
        in_specs=[pl.BlockSpec(memory_space=pltpu.VMEM)] * 2 + [pl.BlockSpec(memory_space=pl.ANY)] * 3,
        out_specs=pl.BlockSpec(memory_space=pltpu.VMEM),
        scratch_shapes=[
            pltpu.VMEM(gate_w.shape, bf16),
            pltpu.VMEM(up_w.shape, bf16),
            pltpu.VMEM(down_w.shape, bf16),
            pltpu.VMEM((groups, 4, capacity, quarter), bf16),
            pltpu.VMEM((groups, 2, 2, capacity, quarter), bf16),
            pltpu.VMEM((groups, 2, capacity, quarter), bf16),
            pltpu.VMEM(send.shape, bf16),
            pltpu.VMEM(send.shape, bf16),
            pltpu.VMEM(send.shape, bf16),
            pltpu.SemaphoreType.DMA((3,)),
            *sems,
        ],
        compiler_params=pltpu.CompilerParams(
            collective_id=0, has_side_effects=True, vmem_limit_bytes=56 * 1024 * 1024
        ),
    )(send, send_cross, gate_w, up_w, down_w)


def shards(tokens, expert_ids, route_weight, norm_gain, expert_gate, expert_up, expert_down):
    groups = lax.axis_size("ep")
    tp_count = lax.axis_size("tp")
    experts = groups * expert_gate.shape[0]
    tok_count, model_width = tokens.shape
    top_count = expert_ids.shape[1]
    capacity = min(tok_count, 3 * tok_count * top_count // experts)
    quarter = model_width // tp_count
    half = groups // 2
    tp = lax.axis_index("tp")
    cross = lax.rem(tp + tp_count // 2, tp_count)

    values = tokens.astype(jnp.float32)
    scale = lax.rsqrt(jnp.mean(values * values, axis=-1, keepdims=True) + NORM_EPS)

    def normed(index):
        own = lax.dynamic_slice_in_dim(tokens, index * quarter, quarter, 1).astype(jnp.float32)
        own_gain = lax.dynamic_slice_in_dim(norm_gain, index * quarter, quarter, 0)
        return (own * scale * own_gain).astype(jnp.bfloat16)

    onehot = expert_ids[:, :, None] == jnp.arange(experts, dtype=jnp.int32)
    named = jnp.any(onehot, axis=1).astype(jnp.bfloat16)
    order = jnp.arange(tok_count, dtype=jnp.int32)
    earlier = (order[None, :] < order[:, None]).astype(jnp.bfloat16)
    slots = jnp.dot(earlier, named, preferred_element_type=jnp.float32).astype(jnp.int32)
    slot_index = jnp.sum(jnp.where(onehot, slots[:, None, :], 0), axis=2)
    position = expert_ids * capacity + slot_index

    def pick(first, count, index):
        slots_here = first * capacity + jnp.arange(count * capacity, dtype=jnp.int32)
        match = position[:, :, None] == slots_here
        picked = lax.dot_general(
            jnp.any(match, axis=1).astype(jnp.bfloat16),
            normed(index),
            (((0,), (0,)), ((), ())),
            preferred_element_type=jnp.float32,
        ).astype(jnp.bfloat16)
        return picked.reshape(count, capacity, quarter), match

    send, match = pick(0, groups, tp)
    send_cross, _ = pick(lax.axis_index("ep") // half * half, half, cross)
    returned = run_experts(
        send, send_cross, expert_gate[0], expert_up[0], expert_down[0]
    ).reshape(experts * capacity, quarter)

    mix = jnp.sum(jnp.where(match, route_weight[:, :, None], 0.0), axis=1)
    high = lax.reduce_precision(mix, 8, 7)
    low = (mix - high).astype(jnp.bfloat16)
    combined = jnp.dot(high.astype(jnp.bfloat16), returned, preferred_element_type=jnp.float32)
    combined += jnp.dot(low, returned, preferred_element_type=jnp.float32)
    return combined.astype(jnp.bfloat16)


def solution(mesh):
    return jax.shard_map(
        shards,
        mesh=mesh,
        in_specs=(
            P("ep", None),
            P("ep", None),
            P("ep", None),
            P(),
            P("ep", None, "tp"),
            P("ep", None, "tp"),
            P("ep", "tp", None),
        ),
        out_specs=P("ep", "tp"),
        check_vma=False,
    )
```

```python
import functools

import jax
import jax.numpy as jnp
from jax import lax
from jax.experimental import pallas as pl
from jax.experimental.pallas import tpu as pltpu
from jax.sharding import PartitionSpec as P

NORM_EPS = 1e-06
CLAMP_LIMIT = 7.0
SWISH_SCALE = 1.702
MESH = pl.DeviceIdType.MESH


def activate(gate_sum, up_sum):
    gate_cut = jnp.minimum(gate_sum, CLAMP_LIMIT)
    up_cut = jnp.clip(up_sum, -CLAMP_LIMIT, CLAMP_LIMIT)
    return ((up_cut + 1.0) * gate_cut * jax.nn.sigmoid(SWISH_SCALE * gate_cut)).astype(jnp.bfloat16)


def expert_kernel(
    groups,
    tokens,
    ids,
    route,
    gain,
    gate_hbm,
    up_hbm,
    down_hbm,
    out,
    gate_w,
    up_w,
    down_w,
    normed_own,
    normed_cross,
    before,
    send,
    send_cross,
    back,
    high,
    low,
    total_out,
    rows,
    part,
    pair_in,
    cross_out,
    cross_in,
    result,
    w_sem,
    disp_send,
    disp_recv,
    cross_send,
    cross_recv,
    core_send,
    core_recv,
    fwd_send,
    fwd_recv,
    pair_send,
    pair_recv,
    sum_send,
    sum_recv,
    ret_send,
    ret_recv,
):
    me = lax.axis_index("ep")
    tp = lax.axis_index("tp")
    a, b = tp // 2, lax.rem(tp, 2)
    cross = 2 * (1 - a) + b
    core = 2 * a + 1 - b
    capacity, quarter = send.shape[1:]
    tok_count = tokens.shape[0]
    half = groups // 2

    weights = [
        pltpu.make_async_copy(src, dst, w_sem.at[i])
        for i, (src, dst) in enumerate(((gate_hbm, gate_w), (up_hbm, up_w), (down_hbm, down_w)))
    ]

    def remote(src, dst, send_sem, recv_sem, ep_index, tp_index):
        return pltpu.make_async_remote_copy(
            src_ref=src,
            dst_ref=dst,
            send_sem=send_sem,
            recv_sem=recv_sem,
            device_id=(ep_index, tp_index),
            device_id_type=MESH,
        )

    def partner(k):
        total, bit = 0, 1
        while bit < groups:
            total += bit * lax.rem(me // bit + k // bit, 2)
            bit *= 2
        return total

    def order(i):
        i = i + (i // (groups - 2)) * (1 - 2 * lax.rem(i, 2))
        return i // 2 + half * lax.rem(i, 2)

    def dispatch(k):
        dst = partner(k)
        return remote(send.at[k], rows.at[k, tp], disp_send.at[k], disp_recv.at[k], dst, tp)

    def dispatch_cross(k):
        dst = partner(k)
        return remote(
            send_cross.at[k],
            rows.at[k, cross],
            cross_send.at[k],
            cross_recv.at[k],
            dst,
            tp,
        )

    def to_cross(k):
        return remote(rows.at[k, tp], rows.at[k, tp], cross_send.at[k], cross_recv.at[k], me, cross)

    def to_core(k):
        return remote(rows.at[k, tp], rows.at[k, tp], core_send.at[k], core_recv.at[k], me, core)

    def forward(k):
        return remote(rows.at[k, cross], rows.at[k, cross], fwd_send.at[k], fwd_recv.at[k], me, core)

    def pair(k):
        return remote(part.at[k, 1 - b], pair_in.at[k], pair_send.at[k], pair_recv.at[k], me, core)

    def cross_sum(k):
        return remote(cross_out.at[k], cross_in.at[k], sum_send.at[k], sum_recv.at[k], me, cross)

    def give_back(k):
        return remote(result.at[k], back.at[k], ret_send.at[k], ret_recv.at[k], partner(k), tp)

    for copy in weights:
        copy.start()

    barrier = pltpu.get_barrier_semaphore()

    def greet(k, carry):
        pl.semaphore_signal(
            barrier, inc=1, device_id=(lax.rem(me + k, groups), tp), device_id_type=MESH
        )
        return carry

    lax.fori_loop(1, groups, greet, 0)
    pl.semaphore_signal(barrier, inc=1, device_id=(me, cross), device_id_type=MESH)
    pl.semaphore_signal(barrier, inc=1, device_id=(me, core), device_id_type=MESH)

    values = tokens[...].astype(jnp.float32)
    scale = lax.rsqrt(jnp.mean(values * values, axis=-1, keepdims=True) + NORM_EPS)

    def normed(index):
        span = pl.ds(pl.multiple_of(index * quarter, quarter), quarter)
        return (tokens[:, span].astype(jnp.float32) * scale * gain[:, span]).astype(jnp.bfloat16)

    normed_own[...] = normed(tp)
    normed_cross[...] = normed(cross)
    earlier = lax.broadcasted_iota(jnp.int32, (tok_count, tok_count), 0)
    later = lax.broadcasted_iota(jnp.int32, (tok_count, tok_count), 1)
    before[...] = jnp.where(earlier < later, 1.0, 0.0).astype(jnp.bfloat16)

    def select(k):
        expert = partner(k)
        hits = ids[...] == expert
        named = jnp.sum(jnp.where(hits, 1.0, 0.0), axis=0, keepdims=True)
        weight = jnp.sum(jnp.where(hits, route[...], 0.0), axis=0, keepdims=True)
        count = jnp.dot(
            jnp.broadcast_to(named, (8, tok_count)).astype(jnp.bfloat16),
            before[...],
            preferred_element_type=jnp.float32,
        )[0:1]
        slot = jnp.where(named > 0.0, count.astype(jnp.int32), -1)
        place = lax.broadcasted_iota(jnp.int32, (capacity, tok_count), 0)
        chosen = place == slot
        mix = jnp.where(chosen, weight, 0.0)
        mix_high = mix.astype(jnp.bfloat16)
        high[k] = mix_high
        low[k] = (mix - mix_high.astype(jnp.float32)).astype(jnp.bfloat16)
        return jnp.where(chosen, 1.0, 0.0).astype(jnp.bfloat16)

    def pick(chosen, source):
        return jnp.dot(chosen, source[...], preferred_element_type=jnp.float32).astype(jnp.bfloat16)

    chosen = select(0)
    rows[0, tp] = pick(chosen, normed_own)
    rows[0, cross] = pick(chosen, normed_cross)
    pl.semaphore_wait(barrier, groups + 1)

    def launch(i, carry):
        k = order(i)
        chosen = select(k)
        send[k] = pick(chosen, normed_own)
        dispatch(k).start()

        @pl.when(k < half)
        def _():
            send_cross[k] = pick(chosen, normed_cross)
            dispatch_cross(k).start()

        return carry

    lax.fori_loop(1, groups, launch, 0)
    for copy in weights:
        copy.wait()

    def step(i, carry):
        @pl.when(i >= 4)
        def _():
            k = order(i - 4)
            cross_sum(k).wait_recv()
            total = part[k, b, a].astype(jnp.float32) + pair_in[k, a].astype(jnp.float32)
            total = (total + cross_in[k].astype(jnp.float32)).astype(jnp.bfloat16)

            @pl.when(k == 0)
            def _():
                back[0] = total

            @pl.when(k > 0)
            def _():
                result[k] = total
                give_back(k).start()

        @pl.when((i >= 3) & (i < groups + 3))
        def _():
            k = order(i - 3)
            pair(k).wait_recv()
            total = part[k, b, 1 - a].astype(jnp.float32) + pair_in[k, 1 - a].astype(jnp.float32)
            cross_out[k] = total.astype(jnp.bfloat16)
            cross_sum(k).start()

        @pl.when((i >= 2) & (i < groups + 2))
        def _():
            k = order(i - 2)
            to_core(k).wait_recv()
            forward(k).wait_recv()
            block = jnp.concatenate([rows[k, j] for j in range(4)], axis=1)
            gate_sum = jnp.dot(block, gate_w[...], preferred_element_type=jnp.float32)
            up_sum = jnp.dot(block, up_w[...], preferred_element_type=jnp.float32)
            activated = activate(gate_sum, up_sum)
            for j in range(4):
                part[k, j % 2, j // 2] = jnp.dot(
                    activated,
                    down_w[:, j * quarter : (j + 1) * quarter],
                    preferred_element_type=jnp.float32,
                ).astype(jnp.bfloat16)
            pair(k).start()

        @pl.when((i >= 1) & (i < groups + 1))
        def _():
            k = order(i - 1)

            @pl.when(k > 0)
            def _():
                to_cross(k).wait_recv()

            forward(k).start()

        @pl.when(i < groups)
        def _():
            k = order(i)

            @pl.when(k > 0)
            def _():
                dispatch(k).wait_recv()

            @pl.when(k >= half)
            def _():
                to_cross(k).start()

            to_core(k).start()

        return carry

    lax.fori_loop(0, groups + 4, step, 0)

    total_out[...] = jnp.zeros_like(total_out)

    def finish(i, carry):
        k = order(i)

        @pl.when(k > 0)
        def _():
            give_back(k).wait_recv()

        for share in (high, low):
            total_out[...] += lax.dot_general(
                share[k], back[k], (((0,), (0,)), ((), ())), preferred_element_type=jnp.float32
            )
        return carry

    lax.fori_loop(0, groups, finish, 0)
    out[...] = total_out[...].astype(jnp.bfloat16)

    def drain(k, carry):
        to_core(k).wait_send()
        forward(k).wait_send()
        pair(k).wait_send()
        cross_sum(k).wait_send()

        @pl.when(k > 0)
        def _():
            to_cross(k).wait_send()
            dispatch(k).wait_send()
            give_back(k).wait_send()

        return carry

    lax.fori_loop(0, groups, drain, 0)


def shards(tokens, expert_ids, route_weight, norm_gain, expert_gate, expert_up, expert_down):
    groups = lax.axis_size("ep")
    tp_count = lax.axis_size("tp")
    experts = groups * expert_gate.shape[0]
    tok_count, model_width = tokens.shape
    top_count = expert_ids.shape[1]
    capacity = min(tok_count, 3 * tok_count * top_count // experts)
    quarter = model_width // tp_count
    bf16 = jnp.bfloat16
    slots = (groups, capacity, quarter)
    weights = (expert_gate[0], expert_up[0], expert_down[0])
    return pl.pallas_call(
        functools.partial(expert_kernel, groups),
        out_shape=jax.ShapeDtypeStruct((tok_count, quarter), bf16),
        in_specs=[pl.BlockSpec(memory_space=pltpu.VMEM)] * 4
        + [pl.BlockSpec(memory_space=pl.ANY)] * 3,
        out_specs=pl.BlockSpec(memory_space=pltpu.VMEM),
        scratch_shapes=[
            *[pltpu.VMEM(weight.shape, bf16) for weight in weights],
            pltpu.VMEM((tok_count, quarter), bf16),
            pltpu.VMEM((tok_count, quarter), bf16),
            pltpu.VMEM((tok_count, tok_count), bf16),
            pltpu.VMEM(slots, bf16),
            pltpu.VMEM((groups // 2, capacity, quarter), bf16),
            pltpu.VMEM(slots, bf16),
            pltpu.VMEM((groups, capacity, tok_count), bf16),
            pltpu.VMEM((groups, capacity, tok_count), bf16),
            pltpu.VMEM((tok_count, quarter), jnp.float32),
            pltpu.VMEM((groups, 4, capacity, quarter), bf16),
            pltpu.VMEM((groups, 2, 2, capacity, quarter), bf16),
            pltpu.VMEM((groups, 2, capacity, quarter), bf16),
            pltpu.VMEM(slots, bf16),
            pltpu.VMEM(slots, bf16),
            pltpu.VMEM(slots, bf16),
            pltpu.SemaphoreType.DMA((3,)),
            *[pltpu.SemaphoreType.DMA((groups,)) for _ in range(14)],
        ],
        compiler_params=pltpu.CompilerParams(
            collective_id=0, has_side_effects=True, vmem_limit_bytes=60 * 1024 * 1024
        ),
    )(tokens, expert_ids.T, route_weight.T, norm_gain[None, :], *weights)


def solution(mesh):
    return jax.shard_map(
        shards,
        mesh=mesh,
        in_specs=(
            P("ep", None),
            P("ep", None),
            P("ep", None),
            P(),
            P("ep", None, "tp"),
            P("ep", None, "tp"),
            P("ep", "tp", None),
        ),
        out_specs=P("ep", "tp"),
        check_vma=False,
    )
```

```python
import functools

import jax
import jax.numpy as jnp
from jax import lax
from jax.experimental import pallas as pl
from jax.experimental.pallas import tpu as pltpu
from jax.sharding import PartitionSpec as P

NORM_EPS = 1e-06
CLAMP_LIMIT = 7.0
SWISH_SCALE = 1.702
MESH = pl.DeviceIdType.MESH


def activate(gate_sum, up_sum):
    gate_cut = jnp.minimum(gate_sum, CLAMP_LIMIT)
    up_cut = jnp.clip(up_sum, -CLAMP_LIMIT, CLAMP_LIMIT)
    return ((up_cut + 1.0) * gate_cut * jax.nn.sigmoid(SWISH_SCALE * gate_cut)).astype(jnp.bfloat16)


def expert_kernel(
    groups,
    tokens,
    ids,
    route,
    gain,
    gate_hbm,
    up_hbm,
    down_hbm,
    out,
    gate_w,
    up_w,
    down_w,
    normed_own,
    normed_cross,
    before,
    raw,
    ids_in,
    ids_send,
    ids_recv,
    send,
    send_cross,
    back,
    high,
    low,
    total_out,
    rows,
    part,
    pair_in,
    cross_out,
    cross_in,
    result,
    w_sem,
    disp_send,
    disp_recv,
    cross_send,
    cross_recv,
    core_send,
    core_recv,
    fwd_send,
    fwd_recv,
    pair_send,
    pair_recv,
    sum_send,
    sum_recv,
    ret_send,
    ret_recv,
):
    me = lax.axis_index("ep")
    tp = lax.axis_index("tp")
    a, b = tp // 2, lax.rem(tp, 2)
    cross = 2 * (1 - a) + b
    core = 2 * a + 1 - b
    capacity, quarter = send.shape[1:]
    tok_count = tokens.shape[0]
    half = groups // 2
    direct = half - 1

    weights = [
        pltpu.make_async_copy(src, dst, w_sem.at[i])
        for i, (src, dst) in enumerate(((gate_hbm, gate_w), (up_hbm, up_w), (down_hbm, down_w)))
    ]

    def remote(src, dst, send_sem, recv_sem, ep_index, tp_index):
        return pltpu.make_async_remote_copy(
            src_ref=src,
            dst_ref=dst,
            send_sem=send_sem,
            recv_sem=recv_sem,
            device_id=(ep_index, tp_index),
            device_id_type=MESH,
        )

    def partner(k):
        total, bit = 0, 1
        while bit < groups:
            total += bit * lax.rem(me // bit + k // bit, 2)
            bit *= 2
        return total

    def order(i):
        i = i + (i // (groups - 2)) * (1 - 2 * lax.rem(i, 2))
        return i // 2 + half * lax.rem(i, 2)

    def dispatch(k):
        dst = partner(k)
        return remote(send.at[k], rows.at[k, tp], disp_send.at[k], disp_recv.at[k], dst, tp)

    def mirror():
        return remote(
            normed_own, raw.at[0], disp_send.at[half], disp_recv.at[half], partner(half), tp
        )

    def relay(k):
        return remote(
            raw.at[0], raw.at[k], disp_send.at[half + k], disp_recv.at[half + k], partner(k), tp
        )

    def tell(k):
        return remote(ids, ids_in.at[k], ids_send.at[k], ids_recv.at[k], partner(half + k), tp)

    def dispatch_cross(k):
        dst = partner(k)
        return remote(
            send_cross.at[k],
            rows.at[k, cross],
            cross_send.at[k],
            cross_recv.at[k],
            dst,
            tp,
        )

    def to_cross(k):
        return remote(rows.at[k, tp], rows.at[k, tp], cross_send.at[k], cross_recv.at[k], me, cross)

    def to_core(k):
        return remote(rows.at[k, tp], rows.at[k, tp], core_send.at[k], core_recv.at[k], me, core)

    def forward(k):
        return remote(rows.at[k, cross], rows.at[k, cross], fwd_send.at[k], fwd_recv.at[k], me, core)

    def pair(k):
        return remote(part.at[k, 1 - b], pair_in.at[k], pair_send.at[k], pair_recv.at[k], me, core)

    def cross_sum(k):
        return remote(cross_out.at[k], cross_in.at[k], sum_send.at[k], sum_recv.at[k], me, cross)

    def give_back(k):
        return remote(result.at[k], back.at[k], ret_send.at[k], ret_recv.at[k], partner(k), tp)

    for copy in weights:
        copy.start()

    barrier = pltpu.get_barrier_semaphore()

    def greet(k, carry):
        pl.semaphore_signal(
            barrier, inc=1, device_id=(lax.rem(me + k, groups), tp), device_id_type=MESH
        )
        return carry

    lax.fori_loop(1, groups, greet, 0)
    pl.semaphore_signal(barrier, inc=1, device_id=(me, cross), device_id_type=MESH)
    pl.semaphore_signal(barrier, inc=1, device_id=(me, core), device_id_type=MESH)

    values = tokens[...].astype(jnp.float32)
    scale = lax.rsqrt(jnp.mean(values * values, axis=-1, keepdims=True) + NORM_EPS)

    def normed(index):
        span = pl.ds(pl.multiple_of(index * quarter, quarter), quarter)
        return (tokens[:, span].astype(jnp.float32) * scale * gain[:, span]).astype(jnp.bfloat16)

    normed_own[...] = normed(tp)
    normed_cross[...] = normed(cross)
    earlier = lax.broadcasted_iota(jnp.int32, (tok_count, tok_count), 0)
    later = lax.broadcasted_iota(jnp.int32, (tok_count, tok_count), 1)
    before[...] = jnp.where(earlier < later, 1.0, 0.0).astype(jnp.bfloat16)

    def locate(id_rows, expert):
        hits = id_rows == expert
        named = jnp.sum(jnp.where(hits, 1.0, 0.0), axis=0, keepdims=True)
        count = jnp.dot(
            jnp.broadcast_to(named, (8, tok_count)).astype(jnp.bfloat16),
            before[...],
            preferred_element_type=jnp.float32,
        )[0:1]
        slot = jnp.where(named > 0.0, count.astype(jnp.int32), -1)
        return hits, lax.broadcasted_iota(jnp.int32, (capacity, tok_count), 0) == slot

    def select(k):
        hits, chosen = locate(ids[...], partner(k))
        weight = jnp.sum(jnp.where(hits, route[...], 0.0), axis=0, keepdims=True)
        mix = jnp.where(chosen, weight, 0.0)
        mix_high = mix.astype(jnp.bfloat16)
        high[k] = mix_high
        low[k] = (mix - mix_high.astype(jnp.float32)).astype(jnp.bfloat16)
        return jnp.where(chosen, 1.0, 0.0).astype(jnp.bfloat16)

    def pick(chosen, source):
        return jnp.dot(chosen, source[...], preferred_element_type=jnp.float32).astype(jnp.bfloat16)

    pl.semaphore_wait(barrier, groups + 1)

    def tell_all(k, carry):
        tell(k).start()
        return carry

    lax.fori_loop(0, half, tell_all, 0)
    mirror().start()
    chosen = select(0)
    rows[0, tp] = pick(chosen, normed_own)
    rows[0, cross] = pick(chosen, normed_cross)

    def launch(k, carry):
        chosen = select(k)
        send[k] = pick(chosen, normed_own)
        dispatch(k).start()

        @pl.when(k < direct)
        def _():
            send_cross[k] = pick(chosen, normed_cross)
            dispatch_cross(k).start()

        return carry

    lax.fori_loop(1, half - 1, launch, 0)
    for copy in weights:
        copy.wait()

    def step(i, carry):
        @pl.when(i >= 4)
        def _():
            k = order(i - 4)
            cross_sum(k).wait_recv()
            total = part[k, b, a].astype(jnp.float32) + pair_in[k, a].astype(jnp.float32)
            total = (total + cross_in[k].astype(jnp.float32)).astype(jnp.bfloat16)

            @pl.when(k == 0)
            def _():
                back[0] = total

            @pl.when(k > 0)
            def _():
                result[k] = total
                give_back(k).start()

        @pl.when((i >= 3) & (i < groups + 3))
        def _():
            k = order(i - 3)
            pair(k).wait_recv()
            total = part[k, b, 1 - a].astype(jnp.float32) + pair_in[k, 1 - a].astype(jnp.float32)
            cross_out[k] = total.astype(jnp.bfloat16)
            cross_sum(k).start()

        @pl.when((i >= 2) & (i < groups + 2))
        def _():
            k = order(i - 2)
            to_core(k).wait_recv()
            forward(k).wait_recv()
            block = jnp.concatenate([rows[k, j] for j in range(4)], axis=1)
            gate_sum = jnp.dot(block, gate_w[...], preferred_element_type=jnp.float32)
            up_sum = jnp.dot(block, up_w[...], preferred_element_type=jnp.float32)
            activated = activate(gate_sum, up_sum)
            for j in range(4):
                part[k, j % 2, j // 2] = jnp.dot(
                    activated,
                    down_w[:, j * quarter : (j + 1) * quarter],
                    preferred_element_type=jnp.float32,
                ).astype(jnp.bfloat16)
            pair(k).start()

        @pl.when((i >= 1) & (i < groups + 1))
        def _():
            k = order(i - 1)

            @pl.when(k > 0)
            def _():
                to_cross(k).wait_recv()

            forward(k).start()

        @pl.when(i < groups)
        def _():
            k = order(i)

            @pl.when((k > 0) & (k < half))
            def _():
                dispatch(k).wait_recv()

            @pl.when(k == half)
            def _():
                mirror().wait_recv()

                def relay_all(j, carry):
                    relay(j).start()
                    return carry

                lax.fori_loop(1, half, relay_all, 0)
                lax.fori_loop(half - 1, half, launch, 0)

            @pl.when(k > half)
            def _():
                relay(k - half).wait_recv()

            @pl.when(k >= half)
            def _():
                select(k)
                tell(k - half).wait_recv()
                _, chosen = locate(ids_in[k - half], me)
                rows[k, tp] = pick(
                    jnp.where(chosen, 1.0, 0.0).astype(jnp.bfloat16), raw.at[k - half]
                )

            @pl.when(k >= direct)
            def _():
                to_cross(k).start()

            to_core(k).start()

        return carry

    lax.fori_loop(0, groups + 4, step, 0)

    total_out[...] = jnp.zeros_like(total_out)

    def finish(i, carry):
        k = order(i)

        @pl.when(k > 0)
        def _():
            give_back(k).wait_recv()

        for share in (high, low):
            total_out[...] += lax.dot_general(
                share[k], back[k], (((0,), (0,)), ((), ())), preferred_element_type=jnp.float32
            )
        return carry

    lax.fori_loop(0, groups, finish, 0)
    out[...] = total_out[...].astype(jnp.bfloat16)

    def drain(k, carry):
        to_core(k).wait_send()
        forward(k).wait_send()
        pair(k).wait_send()
        cross_sum(k).wait_send()

        @pl.when(k > 0)
        def _():
            to_cross(k).wait_send()
            give_back(k).wait_send()

        @pl.when((k > 0) & (k < half))
        def _():
            dispatch(k).wait_send()
            relay(k).wait_send()
            tell(k).wait_send()

        @pl.when(k == 0)
        def _():
            mirror().wait_send()
            tell(0).wait_send()

        return carry

    lax.fori_loop(0, groups, drain, 0)


def shards(tokens, expert_ids, route_weight, norm_gain, expert_gate, expert_up, expert_down):
    groups = lax.axis_size("ep")
    tp_count = lax.axis_size("tp")
    experts = groups * expert_gate.shape[0]
    tok_count, model_width = tokens.shape
    top_count = expert_ids.shape[1]
    capacity = min(tok_count, 3 * tok_count * top_count // experts)
    quarter = model_width // tp_count
    bf16 = jnp.bfloat16
    slots = (groups, capacity, quarter)
    weights = (expert_gate[0], expert_up[0], expert_down[0])
    return pl.pallas_call(
        functools.partial(expert_kernel, groups),
        out_shape=jax.ShapeDtypeStruct((tok_count, quarter), bf16),
        in_specs=[pl.BlockSpec(memory_space=pltpu.VMEM)] * 4
        + [pl.BlockSpec(memory_space=pl.ANY)] * 3,
        out_specs=pl.BlockSpec(memory_space=pltpu.VMEM),
        scratch_shapes=[
            *[pltpu.VMEM(weight.shape, bf16) for weight in weights],
            pltpu.VMEM((tok_count, quarter), bf16),
            pltpu.VMEM((tok_count, quarter), bf16),
            pltpu.VMEM((tok_count, tok_count), bf16),
            pltpu.VMEM((groups // 2, tok_count, quarter), bf16),
            pltpu.VMEM((groups // 2, top_count, tok_count), jnp.int32),
            pltpu.SemaphoreType.DMA((groups // 2,)),
            pltpu.SemaphoreType.DMA((groups // 2,)),
            pltpu.VMEM(slots, bf16),
            pltpu.VMEM((groups // 2, capacity, quarter), bf16),
            pltpu.VMEM(slots, bf16),
            pltpu.VMEM((groups, capacity, tok_count), bf16),
            pltpu.VMEM((groups, capacity, tok_count), bf16),
            pltpu.VMEM((tok_count, quarter), jnp.float32),
            pltpu.VMEM((groups, 4, capacity, quarter), bf16),
            pltpu.VMEM((groups, 2, 2, capacity, quarter), bf16),
            pltpu.VMEM((groups, 2, capacity, quarter), bf16),
            pltpu.VMEM(slots, bf16),
            pltpu.VMEM(slots, bf16),
            pltpu.VMEM(slots, bf16),
            pltpu.SemaphoreType.DMA((3,)),
            *[pltpu.SemaphoreType.DMA((groups,)) for _ in range(14)],
        ],
        compiler_params=pltpu.CompilerParams(
            collective_id=0, has_side_effects=True, vmem_limit_bytes=60 * 1024 * 1024
        ),
    )(tokens, expert_ids.T, route_weight.T, norm_gain[None, :], *weights)


def solution(mesh):
    return jax.shard_map(
        shards,
        mesh=mesh,
        in_specs=(
            P("ep", None),
            P("ep", None),
            P("ep", None),
            P(),
            P("ep", None, "tp"),
            P("ep", None, "tp"),
            P("ep", "tp", None),
        ),
        out_specs=P("ep", "tp"),
        check_vma=False,
    )
```

```python
import functools

import jax
import jax.numpy as jnp
from jax import lax
from jax.experimental import pallas as pl
from jax.experimental.pallas import tpu as pltpu
from jax.sharding import PartitionSpec as P

NORM_EPS = 1e-06
CLAMP_LIMIT = 7.0
SWISH_SCALE = 1.702
MESH = pl.DeviceIdType.MESH


def activate(gate_sum, up_sum):
    gate_cut = jnp.minimum(gate_sum, CLAMP_LIMIT)
    up_cut = jnp.clip(up_sum, -CLAMP_LIMIT, CLAMP_LIMIT)
    return ((up_cut + 1.0) * gate_cut * jax.nn.sigmoid(SWISH_SCALE * gate_cut)).astype(jnp.bfloat16)


def expert_kernel(
    groups,
    tokens,
    ids,
    route,
    gain,
    gate_hbm,
    up_hbm,
    down_hbm,
    out,
    gate_w,
    up_w,
    down_w,
    normed_own,
    normed_cross,
    before,
    send,
    send_cross,
    back,
    high,
    low,
    total_out,
    rows,
    part,
    pair_in,
    cross_out,
    cross_in,
    result,
    w_sem,
    disp_send,
    disp_recv,
    cross_send,
    cross_recv,
    core_send,
    core_recv,
    fwd_send,
    fwd_recv,
    pair_send,
    pair_recv,
    sum_send,
    sum_recv,
    ret_send,
    ret_recv,
):
    me = lax.axis_index("ep")
    tp = lax.axis_index("tp")
    a, b = tp // 2, lax.rem(tp, 2)
    cross = 2 * (1 - a) + b
    core = 2 * a + 1 - b
    capacity, quarter = send.shape[1:]
    tok_count = tokens.shape[0]
    half = groups // 2

    weights = [
        pltpu.make_async_copy(src, dst, w_sem.at[i])
        for i, (src, dst) in enumerate(((gate_hbm, gate_w), (up_hbm, up_w), (down_hbm, down_w)))
    ]

    def remote(src, dst, send_sem, recv_sem, ep_index, tp_index):
        return pltpu.make_async_remote_copy(
            src_ref=src,
            dst_ref=dst,
            send_sem=send_sem,
            recv_sem=recv_sem,
            device_id=(ep_index, tp_index),
            device_id_type=MESH,
        )

    def partner(k):
        total, bit = 0, 1
        while bit < groups:
            total += bit * lax.rem(me // bit + k // bit, 2)
            bit *= 2
        return total

    def order(i):
        i = i + (i // (groups - 2)) * (1 - 2 * lax.rem(i, 2))
        return i // 2 + half * lax.rem(i, 2)

    def dispatch(k):
        dst = partner(k)
        return remote(send.at[k], rows.at[k, tp], disp_send.at[k], disp_recv.at[k], dst, tp)

    def dispatch_cross(k):
        dst = partner(k)
        return remote(
            send_cross.at[k],
            rows.at[k, cross],
            cross_send.at[k],
            cross_recv.at[k],
            dst,
            tp,
        )

    def to_cross(k):
        return remote(rows.at[k, tp], rows.at[k, tp], cross_send.at[k], cross_recv.at[k], me, cross)

    def to_core(k):
        return remote(rows.at[k, tp], rows.at[k, tp], core_send.at[k], core_recv.at[k], me, core)

    def forward(k):
        return remote(rows.at[k, cross], rows.at[k, cross], fwd_send.at[k], fwd_recv.at[k], me, core)

    def pair(k):
        return remote(part.at[k, 1 - b], pair_in.at[k], pair_send.at[k], pair_recv.at[k], me, core)

    def cross_sum(k):
        return remote(cross_out.at[k], cross_in.at[k], sum_send.at[k], sum_recv.at[k], me, cross)

    def give_back(k):
        return remote(result.at[k], back.at[k], ret_send.at[k], ret_recv.at[k], partner(k), tp)

    for copy in weights:
        copy.start()

    barrier = pltpu.get_barrier_semaphore()

    def greet(k, carry):
        pl.semaphore_signal(
            barrier, inc=1, device_id=(lax.rem(me + k, groups), tp), device_id_type=MESH
        )
        return carry

    lax.fori_loop(1, groups, greet, 0)
    pl.semaphore_signal(barrier, inc=1, device_id=(me, cross), device_id_type=MESH)
    pl.semaphore_signal(barrier, inc=1, device_id=(me, core), device_id_type=MESH)

    values = tokens[...].astype(jnp.float32)
    scale = lax.rsqrt(jnp.mean(values * values, axis=-1, keepdims=True) + NORM_EPS)

    def normed(index):
        span = pl.ds(pl.multiple_of(index * quarter, quarter), quarter)
        return (tokens[:, span].astype(jnp.float32) * scale * gain[:, span]).astype(jnp.bfloat16)

    normed_own[...] = normed(tp)
    normed_cross[...] = normed(cross)
    earlier = lax.broadcasted_iota(jnp.int32, (tok_count, tok_count), 0)
    later = lax.broadcasted_iota(jnp.int32, (tok_count, tok_count), 1)
    before[...] = jnp.where(earlier < later, 1.0, 0.0).astype(jnp.bfloat16)

    def select(k):
        expert = partner(k)
        hits = ids[...] == expert
        named = jnp.sum(jnp.where(hits, 1.0, 0.0), axis=0, keepdims=True)
        weight = jnp.sum(jnp.where(hits, route[...], 0.0), axis=0, keepdims=True)
        count = jnp.dot(
            jnp.broadcast_to(named, (8, tok_count)).astype(jnp.bfloat16),
            before[...],
            preferred_element_type=jnp.float32,
        )[0:1]
        slot = jnp.where(named > 0.0, count.astype(jnp.int32), -1)
        place = lax.broadcasted_iota(jnp.int32, (capacity, tok_count), 0)
        chosen = place == slot
        mix = jnp.where(chosen, weight, 0.0)
        mix_high = mix.astype(jnp.bfloat16)
        high[k] = mix_high
        low[k] = (mix - mix_high.astype(jnp.float32)).astype(jnp.bfloat16)
        return jnp.where(chosen, 1.0, 0.0).astype(jnp.bfloat16)

    def pick(chosen, source):
        return jnp.dot(chosen, source[...], preferred_element_type=jnp.float32).astype(jnp.bfloat16)

    chosen = select(0)
    rows[0, tp] = pick(chosen, normed_own)
    rows[0, cross] = pick(chosen, normed_cross)
    pl.semaphore_wait(barrier, groups + 1)

    def launch(i, carry):
        k = order(i)
        chosen = select(k)
        send[k] = pick(chosen, normed_own)
        dispatch(k).start()

        @pl.when(k < half)
        def _():
            send_cross[k] = pick(chosen, normed_cross)
            dispatch_cross(k).start()

        return carry

    lax.fori_loop(1, groups, launch, 0)
    for copy in weights:
        copy.wait()

    def spread(k):
        @pl.when(k > 0)
        def _():
            dispatch(k).wait_recv()

        @pl.when(k >= half)
        def _():
            to_cross(k).start()

        to_core(k).start()

    def pass_on(k):
        @pl.when(k > 0)
        def _():
            to_cross(k).wait_recv()

        forward(k).start()

    def compute(k):
        to_core(k).wait_recv()
        forward(k).wait_recv()
        block = jnp.concatenate([rows[k, j] for j in range(4)], axis=1)
        gate_sum = jnp.dot(block, gate_w[...], preferred_element_type=jnp.float32)
        up_sum = jnp.dot(block, up_w[...], preferred_element_type=jnp.float32)
        activated = activate(gate_sum, up_sum)
        for j in range(4):
            part[k, j % 2, j // 2] = jnp.dot(
                activated,
                down_w[:, j * quarter : (j + 1) * quarter],
                preferred_element_type=jnp.float32,
            ).astype(jnp.bfloat16)
        pair(k).start()

    def add_pair(k):
        pair(k).wait_recv()
        total = part[k, b, 1 - a].astype(jnp.float32) + pair_in[k, 1 - a].astype(jnp.float32)
        cross_out[k] = total.astype(jnp.bfloat16)
        cross_sum(k).start()

    def add_cross(k):
        cross_sum(k).wait_recv()
        total = part[k, b, a].astype(jnp.float32) + pair_in[k, a].astype(jnp.float32)
        total = (total + cross_in[k].astype(jnp.float32)).astype(jnp.bfloat16)

        @pl.when(k == 0)
        def _():
            back[0] = total

        @pl.when(k > 0)
        def _():
            result[k] = total
            give_back(k).start()

    for stage in (spread, pass_on, compute, add_pair):
        stage(0)

    def step(i, carry):
        for stage, lag in ((add_cross, 4), (add_pair, 3), (compute, 2), (pass_on, 1), (spread, 0)):
            first = 1 + lag if lag < 4 else 4

            @pl.when((i >= first) & (i < groups + lag))
            def _():
                stage(order(i - lag))

        return carry

    lax.fori_loop(1, groups + 4, step, 0)

    total_out[...] = jnp.zeros_like(total_out)

    def finish(i, carry):
        k = order(i)

        @pl.when(k > 0)
        def _():
            give_back(k).wait_recv()

        for share in (high, low):
            total_out[...] += lax.dot_general(
                share[k], back[k], (((0,), (0,)), ((), ())), preferred_element_type=jnp.float32
            )
        return carry

    lax.fori_loop(0, groups, finish, 0)
    out[...] = total_out[...].astype(jnp.bfloat16)

    def drain(k, carry):
        to_core(k).wait_send()
        forward(k).wait_send()
        pair(k).wait_send()
        cross_sum(k).wait_send()

        @pl.when(k > 0)
        def _():
            to_cross(k).wait_send()
            dispatch(k).wait_send()
            give_back(k).wait_send()

        return carry

    lax.fori_loop(0, groups, drain, 0)


def shards(tokens, expert_ids, route_weight, norm_gain, expert_gate, expert_up, expert_down):
    groups = lax.axis_size("ep")
    tp_count = lax.axis_size("tp")
    experts = groups * expert_gate.shape[0]
    tok_count, model_width = tokens.shape
    top_count = expert_ids.shape[1]
    capacity = min(tok_count, 3 * tok_count * top_count // experts)
    quarter = model_width // tp_count
    bf16 = jnp.bfloat16
    slots = (groups, capacity, quarter)
    weights = (expert_gate[0], expert_up[0], expert_down[0])
    return pl.pallas_call(
        functools.partial(expert_kernel, groups),
        out_shape=jax.ShapeDtypeStruct((tok_count, quarter), bf16),
        in_specs=[pl.BlockSpec(memory_space=pltpu.VMEM)] * 4
        + [pl.BlockSpec(memory_space=pl.ANY)] * 3,
        out_specs=pl.BlockSpec(memory_space=pltpu.VMEM),
        scratch_shapes=[
            *[pltpu.VMEM(weight.shape, bf16) for weight in weights],
            pltpu.VMEM((tok_count, quarter), bf16),
            pltpu.VMEM((tok_count, quarter), bf16),
            pltpu.VMEM((tok_count, tok_count), bf16),
            pltpu.VMEM(slots, bf16),
            pltpu.VMEM((groups // 2, capacity, quarter), bf16),
            pltpu.VMEM(slots, bf16),
            pltpu.VMEM((groups, capacity, tok_count), bf16),
            pltpu.VMEM((groups, capacity, tok_count), bf16),
            pltpu.VMEM((tok_count, quarter), jnp.float32),
            pltpu.VMEM((groups, 4, capacity, quarter), bf16),
            pltpu.VMEM((groups, 2, 2, capacity, quarter), bf16),
            pltpu.VMEM((groups, 2, capacity, quarter), bf16),
            pltpu.VMEM(slots, bf16),
            pltpu.VMEM(slots, bf16),
            pltpu.VMEM(slots, bf16),
            pltpu.SemaphoreType.DMA((3,)),
            *[pltpu.SemaphoreType.DMA((groups,)) for _ in range(14)],
        ],
        compiler_params=pltpu.CompilerParams(
            collective_id=0, has_side_effects=True, vmem_limit_bytes=60 * 1024 * 1024
        ),
    )(tokens, expert_ids.T, route_weight.T, norm_gain[None, :], *weights)


def solution(mesh):
    return jax.shard_map(
        shards,
        mesh=mesh,
        in_specs=(
            P("ep", None),
            P("ep", None),
            P("ep", None),
            P(),
            P("ep", None, "tp"),
            P("ep", None, "tp"),
            P("ep", "tp", None),
        ),
        out_specs=P("ep", "tp"),
        check_vma=False,
    )
```

```python
import functools

import jax
import jax.numpy as jnp
from jax import lax
from jax.experimental import pallas as pl
from jax.experimental.pallas import tpu as pltpu
from jax.sharding import PartitionSpec as P

NORM_EPS = 1e-06
CLAMP_LIMIT = 7.0
SWISH_SCALE = 1.702
MESH = pl.DeviceIdType.MESH


def activate(gate_sum, up_sum):
    gate_cut = jnp.minimum(gate_sum, CLAMP_LIMIT)
    up_cut = jnp.clip(up_sum, -CLAMP_LIMIT, CLAMP_LIMIT)
    return ((up_cut + 1.0) * gate_cut * jax.nn.sigmoid(SWISH_SCALE * gate_cut)).astype(jnp.bfloat16)


def expert_kernel(
    groups,
    tokens,
    ids,
    route,
    gain,
    gate_hbm,
    up_hbm,
    down_hbm,
    out,
    gate_w,
    up_w,
    down_w,
    normed_own,
    normed_cross,
    before,
    send,
    send_cross,
    back,
    high,
    low,
    total_out,
    rows,
    part,
    pair_in,
    cross_out,
    cross_in,
    result,
    w_sem,
    disp_send,
    disp_recv,
    cross_send,
    cross_recv,
    core_send,
    core_recv,
    fwd_send,
    fwd_recv,
    pair_send,
    pair_recv,
    sum_send,
    sum_recv,
    ret_send,
    ret_recv,
):
    me = lax.axis_index("ep")
    tp = lax.axis_index("tp")
    a, b = tp // 2, lax.rem(tp, 2)
    cross = 2 * (1 - a) + b
    core = 2 * a + 1 - b
    capacity, quarter = send.shape[1:]
    tok_count = tokens.shape[0]
    half = groups // 2

    weights = [
        pltpu.make_async_copy(src, dst, w_sem.at[i])
        for i, (src, dst) in enumerate(((gate_hbm, gate_w), (up_hbm, up_w), (down_hbm, down_w)))
    ]

    def remote(src, dst, send_sem, recv_sem, ep_index, tp_index):
        return pltpu.make_async_remote_copy(
            src_ref=src,
            dst_ref=dst,
            send_sem=send_sem,
            recv_sem=recv_sem,
            device_id=(ep_index, tp_index),
            device_id_type=MESH,
        )

    def partner(k):
        total, bit = 0, 1
        while bit < groups:
            total += bit * lax.rem(me // bit + k // bit, 2)
            bit *= 2
        return total

    def order(i):
        i = i + (i // (groups - 2)) * (1 - 2 * lax.rem(i, 2))
        return i // 2 + half * lax.rem(i, 2)

    def dispatch(k):
        dst = partner(k)
        return remote(send.at[k], rows.at[k, tp], disp_send.at[k], disp_recv.at[k], dst, tp)

    def dispatch_cross(k):
        dst = partner(k)
        return remote(
            send_cross.at[k],
            rows.at[k, cross],
            cross_send.at[k],
            cross_recv.at[k],
            dst,
            tp,
        )

    def to_cross(k):
        return remote(rows.at[k, tp], rows.at[k, tp], cross_send.at[k], cross_recv.at[k], me, cross)

    def to_core(k):
        return remote(rows.at[k, tp], rows.at[k, tp], core_send.at[k], core_recv.at[k], me, core)

    def forward(k):
        return remote(rows.at[k, cross], rows.at[k, cross], fwd_send.at[k], fwd_recv.at[k], me, core)

    def pair(k):
        return remote(part.at[k, 1 - b], pair_in.at[k], pair_send.at[k], pair_recv.at[k], me, core)

    def cross_sum(k):
        return remote(cross_out.at[k], cross_in.at[k], sum_send.at[k], sum_recv.at[k], me, cross)

    def give_back(k):
        return remote(result.at[k], back.at[k], ret_send.at[k], ret_recv.at[k], partner(k), tp)

    for copy in weights:
        copy.start()

    barrier = pltpu.get_barrier_semaphore()

    def greet(k, carry):
        pl.semaphore_signal(
            barrier, inc=1, device_id=(lax.rem(me + k, groups), tp), device_id_type=MESH
        )
        return carry

    lax.fori_loop(1, groups, greet, 0)
    pl.semaphore_signal(barrier, inc=1, device_id=(me, cross), device_id_type=MESH)
    pl.semaphore_signal(barrier, inc=1, device_id=(me, core), device_id_type=MESH)

    values = tokens[...].astype(jnp.float32)
    scale = lax.rsqrt(jnp.mean(values * values, axis=-1, keepdims=True) + NORM_EPS)

    def normed(index):
        span = pl.ds(pl.multiple_of(index * quarter, quarter), quarter)
        return (tokens[:, span].astype(jnp.float32) * scale * gain[:, span]).astype(jnp.bfloat16)

    normed_own[...] = normed(tp)
    normed_cross[...] = normed(cross)
    earlier = lax.broadcasted_iota(jnp.int32, (tok_count, tok_count), 0)
    later = lax.broadcasted_iota(jnp.int32, (tok_count, tok_count), 1)
    before[...] = jnp.where(earlier < later, 1.0, 0.0).astype(jnp.bfloat16)

    def select(k):
        expert = partner(k)
        hits = ids[...] == expert
        named = jnp.sum(jnp.where(hits, 1.0, 0.0), axis=0, keepdims=True)
        weight = jnp.sum(jnp.where(hits, route[...], 0.0), axis=0, keepdims=True)
        count = jnp.dot(
            jnp.broadcast_to(named, (8, tok_count)).astype(jnp.bfloat16),
            before[...],
            preferred_element_type=jnp.float32,
        )[0:1]
        slot = jnp.where(named > 0.0, count.astype(jnp.int32), -1)
        place = lax.broadcasted_iota(jnp.int32, (capacity, tok_count), 0)
        chosen = place == slot
        mix = jnp.where(chosen, weight, 0.0)
        mix_high = mix.astype(jnp.bfloat16)
        high[k] = mix_high
        low[k] = (mix - mix_high.astype(jnp.float32)).astype(jnp.bfloat16)
        return jnp.where(chosen, 1.0, 0.0).astype(jnp.bfloat16)

    def pick(chosen, source):
        return jnp.dot(chosen, source[...], preferred_element_type=jnp.float32).astype(jnp.bfloat16)

    chosen = select(0)
    rows[0, tp] = pick(chosen, normed_own)
    rows[0, cross] = pick(chosen, normed_cross)
    pl.semaphore_wait(barrier, groups + 1)

    def launch(i, carry):
        k = order(i)
        chosen = select(k)
        send[k] = pick(chosen, normed_own)
        dispatch(k).start()

        @pl.when(k < half)
        def _():
            send_cross[k] = pick(chosen, normed_cross)
            dispatch_cross(k).start()

        return carry

    lax.fori_loop(1, groups, launch, 0)
    for copy in weights:
        copy.wait()

    def step(i, carry):
        @pl.when(i >= 4)
        def _():
            k = order(i - 4)
            cross_sum(k).wait_recv()
            total = part[k, b, a].astype(jnp.float32) + pair_in[k, a].astype(jnp.float32)
            total = (total + cross_in[k].astype(jnp.float32)).astype(jnp.bfloat16)

            @pl.when(k == 0)
            def _():
                back[0] = total

            @pl.when(k > 0)
            def _():
                result[k] = total
                give_back(k).start()

        @pl.when((i >= 3) & (i < groups + 3))
        def _():
            k = order(i - 3)
            pair(k).wait_recv()
            total = part[k, b, 1 - a].astype(jnp.float32) + pair_in[k, 1 - a].astype(jnp.float32)
            cross_out[k] = total.astype(jnp.bfloat16)
            cross_sum(k).start()

        @pl.when((i >= 1) & (i < groups + 1))
        def _():
            k = order(i - 1)

            @pl.when(k > 0)
            def _():
                to_cross(k).wait_recv()

            forward(k).start()

        @pl.when(i < groups)
        def _():
            k = order(i)

            @pl.when(k > 0)
            def _():
                dispatch(k).wait_recv()

            @pl.when(k >= half)
            def _():
                to_cross(k).start()

            to_core(k).start()

        @pl.when((i >= 2) & (i < groups + 2))
        def _():
            k = order(i - 2)
            to_core(k).wait_recv()
            forward(k).wait_recv()
            block = jnp.concatenate([rows[k, j] for j in range(4)], axis=1)
            gate_sum = jnp.dot(block, gate_w[...], preferred_element_type=jnp.float32)
            up_sum = jnp.dot(block, up_w[...], preferred_element_type=jnp.float32)
            activated = activate(gate_sum, up_sum)
            for j in range(4):
                part[k, j % 2, j // 2] = jnp.dot(
                    activated,
                    down_w[:, j * quarter : (j + 1) * quarter],
                    preferred_element_type=jnp.float32,
                ).astype(jnp.bfloat16)
            pair(k).start()

        return carry

    lax.fori_loop(0, groups + 4, step, 0)

    total_out[...] = jnp.zeros_like(total_out)

    def finish(i, carry):
        k = order(i)

        @pl.when(k > 0)
        def _():
            give_back(k).wait_recv()

        for share in (high, low):
            total_out[...] += lax.dot_general(
                share[k], back[k], (((0,), (0,)), ((), ())), preferred_element_type=jnp.float32
            )
        return carry

    lax.fori_loop(0, groups, finish, 0)
    out[...] = total_out[...].astype(jnp.bfloat16)

    def drain(k, carry):
        to_core(k).wait_send()
        forward(k).wait_send()
        pair(k).wait_send()
        cross_sum(k).wait_send()

        @pl.when(k > 0)
        def _():
            to_cross(k).wait_send()
            dispatch(k).wait_send()
            give_back(k).wait_send()

        return carry

    lax.fori_loop(0, groups, drain, 0)


def shards(tokens, expert_ids, route_weight, norm_gain, expert_gate, expert_up, expert_down):
    groups = lax.axis_size("ep")
    tp_count = lax.axis_size("tp")
    experts = groups * expert_gate.shape[0]
    tok_count, model_width = tokens.shape
    top_count = expert_ids.shape[1]
    capacity = min(tok_count, 3 * tok_count * top_count // experts)
    quarter = model_width // tp_count
    bf16 = jnp.bfloat16
    slots = (groups, capacity, quarter)
    weights = (expert_gate[0], expert_up[0], expert_down[0])
    return pl.pallas_call(
        functools.partial(expert_kernel, groups),
        out_shape=jax.ShapeDtypeStruct((tok_count, quarter), bf16),
        in_specs=[pl.BlockSpec(memory_space=pltpu.VMEM)] * 4
        + [pl.BlockSpec(memory_space=pl.ANY)] * 3,
        out_specs=pl.BlockSpec(memory_space=pltpu.VMEM),
        scratch_shapes=[
            *[pltpu.VMEM(weight.shape, bf16) for weight in weights],
            pltpu.VMEM((tok_count, quarter), bf16),
            pltpu.VMEM((tok_count, quarter), bf16),
            pltpu.VMEM((tok_count, tok_count), bf16),
            pltpu.VMEM(slots, bf16),
            pltpu.VMEM((groups // 2, capacity, quarter), bf16),
            pltpu.VMEM(slots, bf16),
            pltpu.VMEM((groups, capacity, tok_count), bf16),
            pltpu.VMEM((groups, capacity, tok_count), bf16),
            pltpu.VMEM((tok_count, quarter), jnp.float32),
            pltpu.VMEM((groups, 4, capacity, quarter), bf16),
            pltpu.VMEM((groups, 2, 2, capacity, quarter), bf16),
            pltpu.VMEM((groups, 2, capacity, quarter), bf16),
            pltpu.VMEM(slots, bf16),
            pltpu.VMEM(slots, bf16),
            pltpu.VMEM(slots, bf16),
            pltpu.SemaphoreType.DMA((3,)),
            *[pltpu.SemaphoreType.DMA((groups,)) for _ in range(14)],
        ],
        compiler_params=pltpu.CompilerParams(
            collective_id=0, has_side_effects=True, vmem_limit_bytes=60 * 1024 * 1024
        ),
    )(tokens, expert_ids.T, route_weight.T, norm_gain[None, :], *weights)


def solution(mesh):
    return jax.shard_map(
        shards,
        mesh=mesh,
        in_specs=(
            P("ep", None),
            P("ep", None),
            P("ep", None),
            P(),
            P("ep", None, "tp"),
            P("ep", None, "tp"),
            P("ep", "tp", None),
        ),
        out_specs=P("ep", "tp"),
        check_vma=False,
    )
```
